256 devices in a mesh: ep: 128 (over z, y, x), tp: 2 (over core).
Axes of the slice: x: 4, y: 4, z: 8, core: 2. Of those that a mesh axis runs over, the one named last changes fastest.
Arguments:
- tokens: bfloat16 [2048, 1024], P('ep'), may hold values from -6 to 6
- lengths: int32 [2048], P('ep'), may hold values from 1 to 1024, 1048576 in all
- routes: int32 [2048, 2], replicated, may hold values from 0 to 15, all different within a row; in each aligned block of 16 rows (0 to 15, 16 to 31, ...) at most 4 rows name the same one
- route_weights: float32 [2048, 2], replicated, may hold values from 0.1 to 1
- key_cache: bfloat16 [2048, 1024, 256], P('ep', None, 'tp'), may hold values from -6 to 6
- value_cache: bfloat16 [2048, 1024, 256], P('ep', None, 'tp'), may hold values from -6 to 6
- w_query: bfloat16 [1024, 1024], P(None, 'tp'), may hold values from -0.1875 to 0.1875
- w_key: bfloat16 [1024, 256], P(None, 'tp'), may hold values from -0.1875 to 0.1875
- w_value: bfloat16 [1024, 256], P(None, 'tp'), may hold values from -0.1875 to 0.1875
- w_out: bfloat16 [1024, 1024], P('tp'), may hold values from -0.1875 to 0.1875
- score_offset: float32 [16], P('tp'), may hold values from -9 to -3
- attn_gain: float32 [1024], replicated, may hold values from 0.1 to 1.9
- ffn_gain: float32 [1024], replicated, may hold values from 0.1 to 1.9
- w_gate: bfloat16 [1024, 114688], P(None, ('ep', 'tp')), may hold values from -0.1875 to 0.1875
- w_up: bfloat16 [1024, 114688], P(None, ('ep', 'tp')), may hold values from -0.1875 to 0.1875
- w_down: bfloat16 [114688, 1024], P(('ep', 'tp')), may hold values from -0.0625 to 0.0625
Outputs:
- layer_out: bfloat16 [2048, 1024], P('ep', 'tp')
- new_keys: bfloat16 [2048, 256], P('ep', 'tp')
- new_values: bfloat16 [2048, 256], P('ep', 'tp')
The draws below stay inside these ranges and needn't reach their ends.
Inputs may be any that keep to these rules, and one draw needn't show every extreme that they name: `routes`: each row names 2 different experts. Among the rows of one index of ep (aligned blocks of 16 rows) no expert is named by more than 4 rows, and in some block one expert is named by exactly 4 rows.
All inputs are finite; a program needn't handle non-finite values. No bound on the sum of `lengths` on one device may be relied on, other than what follows from the above.
Results may differ from the reference program's by a relative error of at most 0.0095.
Values may be sent and summed in bfloat16 or wider, within the bound.
No kernel may reach another device: no remote copies, remote signals or barrier semaphores. Data moves between devices by JAX's collectives and lax.ppermute only.
A program may use at most 128 MiB of HBM per device.

```python
import math
import jax
import jax.numpy as jnp
import numpy as np
from jax import lax

D = 1024
HEADS = 16
KV_HEADS = 4
HEAD_DIM = 64
EXP_WIDTH = 7168
EXPERTS = 16
TOPK = 2
SEQ_DEV = 16
CTX = 1024
TOKENS = 2048
CAP = 4
N_EP = 128


def draw_score_offset(key, part):
    chooser = jax.random.fold_in(key, 11)
    slow_key = jax.random.fold_in(key, 12)
    fast_key = jax.random.fold_in(key, 13)
    slow_heads = jax.random.bernoulli(chooser, 0.5, (HEADS,))
    slow_values = jax.random.uniform(slow_key, (HEADS,), jnp.float32, -8.0, -7.0)
    fast_values = jax.random.uniform(fast_key, (HEADS,), jnp.float32, -4.0, -3.0)
    return jnp.where(slow_heads, slow_values, fast_values)


def block_levels(stream_key, dims, shards, low, largest):
    def one(position, blocks):
        steps = jax.random.uniform(jax.random.fold_in(jax.random.fold_in(stream_key, 6), position), (blocks,), jnp.float32, low / len(shards), largest / len(shards))
        return jnp.repeat(jnp.exp(steps), dims[position] // blocks).reshape((-1,) + (1,) * (len(dims) - position - 1))

    level = one(*shards[0])
    for cut in shards[1:]:
        level = level * one(*cut)
    return level


def length_profile(number_of, total, bound, slope):
    weights = [(1 << 20) // math.isqrt(standing ** slope) + 1 for standing in range(2, number_of + 1)]
    spare, holding = total - bound - (number_of - 1), [1] * (number_of - 1)
    while spare > 0:
        candidates = [i for i in range(number_of - 1) if holding[i] < bound]
        whole, remaining = sum([weights[i] for i in candidates]), spare
        for i in candidates:
            extra = min(bound - holding[i], max(1, remaining * weights[i] // whole), spare)
            holding[i] = holding[i] + extra
            spare = spare - extra
    return np.array([bound] + holding)


def uneven_parts(own_key, amount, total, limit, skew):
    if amount == 2:
        one = jax.random.randint(own_key, (), max(1, total - limit), min(limit, total - 1) + 1)
        return jnp.stack([one, total - one])
    sizes = jnp.asarray(length_profile(amount, total, limit, skew), jnp.int32)
    pairs = (amount - 1) // 2
    donor, receiver = sizes[1:1 + 2 * pairs:2], sizes[2:2 + 2 * pairs:2]
    slack = jnp.minimum(donor - 1, limit - receiver)
    shifted = jax.random.randint(jax.random.fold_in(own_key, 1), (pairs,), 0, 1 << 20) % (slack + 1)
    sizes = sizes.at[1:1 + 2 * pairs:2].set(donor - shifted).at[2:2 + 2 * pairs:2].set(receiver + shifted)
    return sizes[jax.random.permutation(jax.random.fold_in(own_key, 2), amount)]


def shared_out(key, own, number, rows, number_of, top, bound, lean):
    order = jax.random.permutation(key, number_of)
    heavy_load, common = portions_of(number_of, rows * top, bound, lean, True), portions_of(number_of, rows * top, bound, lean, False)
    places = jnp.arange(number_of)

    def named(sizes, turn):
        used = int((sizes > 0).sum())
        fixed = max(1, used // 4)
        shifted = fixed + (places - fixed + turn * (used - fixed)) % max(1, number_of - fixed)
        return jnp.zeros((number_of,), jnp.int32).at[order[jnp.where(places < fixed, places, shifted)]].set(jnp.asarray(sizes, jnp.int32))

    sizes = jnp.where(number % 4 == 0, named(heavy_load, number // 4), named(common, number - number // 4 - 1))
    mixed = jax.random.permutation(jax.random.fold_in(own, 3), number_of)
    source_of, taker = mixed[0:number_of // 2 * 2:2], mixed[1:number_of // 2 * 2:2]
    margin = jnp.minimum(sizes[source_of] - 1, bound - sizes[taker]) // 2
    margin = jnp.where((source_of == order[0]) | (taker == order[0]) | (sizes[taker] == 0), 0, jnp.maximum(margin, 0))
    shifted = jax.random.randint(jax.random.fold_in(own, 4), (number_of // 2,), 0, 1 << 20) % (margin + 1)
    sizes = sizes.at[source_of].add(-shifted).at[taker].add(shifted)
    members = jnp.searchsorted(jnp.cumsum(sizes), jnp.arange(rows * top), side="right").astype(jnp.int32)
    listing = members.reshape(top, rows).T
    listing = listing[jax.random.permutation(jax.random.fold_in(own, 1), rows)]
    turn = jax.random.randint(jax.random.fold_in(own, 2), (rows, 1), 0, top)
    return jnp.take_along_axis(listing, (jnp.arange(top)[None, :] + turn) % top, axis=1)


def portions_of(amount, total, bound, skew, full):
    portions = [(1 << 20) // math.isqrt(grade ** skew) + 1 for grade in range(1, amount + 1)]
    largest = bound if full else min(bound, max(-(-total // amount), total * portions[0] // sum(portions)))
    least = 1 if total - largest >= amount - 1 else 0
    given, surplus = [largest] + [least] * (amount - 1), total - largest - least * (amount - 1)
    while surplus > 0:
        free = [i for i in range(1, amount) if given[i] < largest] or [i for i in range(1, amount) if given[i] < bound]
        whole, budget = sum([portions[i] for i in free]), surplus
        for i in free:
            more = min(bound - given[i], max(1, budget * portions[i] // whole), surplus)
            given[i] = given[i] + more
            surplus = surplus - more
    return np.array(given)


def bell_draw(own_key, shape, scale, limit, pieces=(), kind=jnp.bfloat16):
    result = scale * jax.random.normal(own_key, shape, jnp.float32)
    if pieces:
        result = result * block_levels(own_key, shape, pieces, -0.22, 0.18)
    return jnp.clip(result, -limit, limit).astype(kind)


def setup_inputs(seed: int = 0) -> dict:
    arg_keys = jax.random.split(jax.random.key(seed), 17)
    tokens = bell_draw(arg_keys[0], (TOKENS, D), 1.0, 6.0, ((0, 128),))
    lengths = uneven_parts(arg_keys[1], TOKENS, TOKENS * CTX // 2, CTX, 2).astype(jnp.int32)
    routes_keys = jax.random.split(jax.random.fold_in(arg_keys[2], 1), TOKENS // SEQ_DEV)
    routes_turns = jax.random.permutation(jax.random.fold_in(arg_keys[2], 3), TOKENS // SEQ_DEV)
    routes = jax.vmap(lambda own, number: shared_out(jax.random.fold_in(arg_keys[2], 2), own, number, SEQ_DEV, EXPERTS, TOPK, CAP, 2))(routes_keys, routes_turns).reshape((TOKENS, TOPK))
    route_weights = jnp.clip(jax.random.uniform(arg_keys[3], (TOKENS, TOPK), jnp.float32, 0.1, 1.0), 0.1, 1.0)
    key_cache = bell_draw(arg_keys[4], (TOKENS, CTX, KV_HEADS * HEAD_DIM), 1.0, 6.0, ((0, 128), (2, 2)))
    value_cache = bell_draw(arg_keys[5], (TOKENS, CTX, KV_HEADS * HEAD_DIM), 1.0, 6.0, ((0, 128), (2, 2)))
    w_query = bell_draw(arg_keys[6], (D, HEADS * HEAD_DIM), D ** -0.5, 0.1875, ((1, 2),))
    w_key = bell_draw(arg_keys[7], (D, KV_HEADS * HEAD_DIM), D ** -0.5, 0.1875, ((1, 2),))
    w_value = bell_draw(arg_keys[8], (D, KV_HEADS * HEAD_DIM), D ** -0.5, 0.1875, ((1, 2),))
    w_out = bell_draw(arg_keys[9], (HEADS * HEAD_DIM, D), (HEADS * HEAD_DIM) ** -0.5, 0.1875, ((0, 2),))
    score_offset = draw_score_offset(jax.random.fold_in(arg_keys[16], 71), 0)
    attn_gain = jnp.clip(1.0 + 0.18 * jax.random.normal(arg_keys[11], (D,), jnp.float32), 0.1, 1.9)
    ffn_gain = jnp.clip(1.0 + 0.18 * jax.random.normal(arg_keys[12], (D,), jnp.float32), 0.1, 1.9)
    w_gate = bell_draw(arg_keys[13], (D, EXPERTS * EXP_WIDTH), D ** -0.5, 0.1875, ((1, 256),))
    w_up = bell_draw(arg_keys[14], (D, EXPERTS * EXP_WIDTH), D ** -0.5, 0.1875, ((1, 256),))
    w_down = bell_draw(arg_keys[15], (EXPERTS * EXP_WIDTH, D), EXP_WIDTH ** -0.5, 0.0625, ((0, 256),))
    return {"tokens": tokens, "lengths": lengths, "routes": routes, "route_weights": route_weights, "key_cache": key_cache, "value_cache": value_cache, "w_query": w_query, "w_key": w_key, "w_value": w_value, "w_out": w_out, "score_offset": score_offset, "attn_gain": attn_gain, "ffn_gain": ffn_gain, "w_gate": w_gate, "w_up": w_up, "w_down": w_down}


norm_eps = 1e-06

def rms_rows(values, gain_row):
    widened = values.astype(jnp.float32)
    scaled = widened * lax.rsqrt(lax.optimization_barrier(jnp.mean(widened * widened, axis=-1, keepdims=True)) + norm_eps)
    return (scaled * gain_row).astype(jnp.bfloat16)

def expert_rows(inputs, gate_cols, up_cols, down_rows):
    gate = jnp.dot(inputs, gate_cols, preferred_element_type=jnp.float32)
    upward = jnp.dot(inputs, up_cols, preferred_element_type=jnp.float32)
    hidden = (jax.nn.silu(gate) * upward).astype(jnp.bfloat16)
    return jnp.dot(hidden, down_rows, preferred_element_type=jnp.float32)

def reference(tokens, lengths, routes, route_weights, key_cache, value_cache, w_query, w_key, w_value, w_out, score_offset, attn_gain, ffn_gain, w_gate, w_up, w_down):
    normed = rms_rows(tokens, attn_gain)
    queries = jnp.dot(normed, w_query, preferred_element_type=jnp.float32).astype(jnp.bfloat16)
    new_keys = jnp.dot(normed, w_key, preferred_element_type=jnp.float32).astype(jnp.bfloat16)
    new_values = jnp.dot(normed, w_value, preferred_element_type=jnp.float32).astype(jnp.bfloat16)
    group_size = HEADS // KV_HEADS
    offsets = score_offset.reshape(KV_HEADS, group_size)[None, :, :, None]

    def attend(blocks):
        query_block, key_block, value_block, length_block = blocks
        count_rows = query_block.shape[0]
        query_heads = query_block.reshape(count_rows, KV_HEADS, group_size, HEAD_DIM).astype(jnp.float32)
        key_heads = key_block.reshape(count_rows, CTX, KV_HEADS, HEAD_DIM).astype(jnp.float32)
        value_heads = value_block.reshape(count_rows, CTX, KV_HEADS, HEAD_DIM).astype(jnp.float32)
        scores = jnp.einsum('bkgd,bskd->bkgs', query_heads, key_heads, precision=lax.Precision.HIGHEST) * HEAD_DIM ** (-0.5) + offsets
        valid = jnp.arange(CTX, dtype=jnp.int32)[None, None, None, :] < length_block[:, None, None, None]
        log_fail = jnp.where(valid, jax.nn.log_sigmoid(-scores), 0.0)
        after = lax.cumsum(log_fail, axis=3, reverse=True) - log_fail
        stick = jnp.where(valid, jnp.exp(jax.nn.log_sigmoid(scores) + after), 0.0).astype(jnp.bfloat16)
        output = jnp.einsum('bkgs,bskd->bkgd', stick.astype(jnp.float32), value_heads, precision=lax.Precision.HIGHEST)
        return output.astype(jnp.bfloat16).reshape(count_rows, HEADS * HEAD_DIM)
    attended = lax.map(attend, (queries.reshape(N_EP, SEQ_DEV, HEADS * HEAD_DIM), key_cache.reshape(N_EP, SEQ_DEV, CTX, KV_HEADS * HEAD_DIM), value_cache.reshape(N_EP, SEQ_DEV, CTX, KV_HEADS * HEAD_DIM), lengths.reshape(N_EP, SEQ_DEV)))
    attended = attended.reshape(TOKENS, HEADS * HEAD_DIM)
    per_half = HEADS * HEAD_DIM // 2
    running = tokens.astype(jnp.float32)
    for half_index in range(2):
        partial_part = jnp.dot(attended[:, half_index * per_half:(half_index + 1) * per_half], w_out[half_index * per_half:(half_index + 1) * per_half], preferred_element_type=jnp.float32)
        rounded = lax.optimization_barrier(partial_part.astype(jnp.bfloat16))
        running = running + rounded.astype(jnp.float32)
    middle = running.astype(jnp.bfloat16)
    moe_in = rms_rows(middle, ffn_gain)
    flat_routes = routes.reshape(-1)
    flat_weights = route_weights.reshape(-1)
    most_rows = N_EP * CAP

    def per_expert(mixture, expert):
        chosen = flat_routes == expert
        picked = jnp.nonzero(chosen, size=most_rows, fill_value=0)[0].astype(jnp.int32)
        filled_count = jnp.sum(chosen.astype(jnp.int32))
        filled = jnp.arange(most_rows, dtype=jnp.int32) < filled_count
        token_rows = (picked // TOPK).astype(jnp.int32)
        chosen_rows = moe_in[token_rows]
        start = (expert * EXP_WIDTH).astype(jnp.int32)
        gate_cols = lax.dynamic_slice_in_dim(w_gate, start, EXP_WIDTH, 1)
        up_cols = lax.dynamic_slice_in_dim(w_up, start, EXP_WIDTH, 1)
        down_rows = lax.dynamic_slice_in_dim(w_down, start, EXP_WIDTH, 0)
        outputs = expert_rows(chosen_rows, gate_cols, up_cols, down_rows)
        scale = jnp.where(filled, flat_weights[picked], 0.0)
        return (mixture.at[token_rows].add(scale[:, None] * outputs), None)
    mixture, _ = lax.scan(per_expert, jnp.zeros((TOKENS, D), jnp.float32), jnp.arange(EXPERTS, dtype=jnp.int32))
    layer_out = (middle.astype(jnp.float32) + mixture).astype(jnp.bfloat16)
    return (layer_out, new_keys, new_values)
```

```python
import jax
import jax.numpy as jnp
from jax import lax
from jax.experimental import pallas as pl
from jax.experimental.pallas import tpu as pltpu
from jax.sharding import PartitionSpec as P

HEAD_DIM = 64
EXPERTS = 16
LANES = 128
norm_eps = 1e-06

f32 = jnp.float32
bf16 = jnp.bfloat16


def rms_rows(values, gain_row):
    widened = values.astype(f32)
    scaled = widened * lax.rsqrt(jnp.mean(widened * widened, axis=-1, keepdims=True) + norm_eps)
    return (scaled * gain_row).astype(bf16)


def dot(a, b, dims=((1,), (0,))):
    return lax.dot_general(a, b, (dims, ((), ())), preferred_element_type=f32)


def split_two(x):
    high = x.astype(bf16)
    return high, (x - high.astype(f32)).astype(bf16)


def iota(shape, dim):
    return lax.broadcasted_iota(jnp.int32, shape, dim)


def attention_kernel(
    lengths_hbm,
    offsets_hbm,
    tokens_hbm,
    gain_hbm,
    key_hbm,
    value_hbm,
    wq_hbm,
    wk_hbm,
    wv_hbm,
    wo_hbm,
    part_out,
    keys_out,
    values_out,
    lengths,
    offsets,
    tokens,
    gain,
    kbuf,
    vbuf,
    wq,
    wk,
    wv,
    wo,
    qrows,
    arows,
    wsem,
    ksem,
    vsem,
):
    seqs, context, width = kbuf.shape
    heads = qrows.shape[0] // seqs
    pairs = seqs // 2
    blocks = context // LANES

    def key_copy(p):
        return pltpu.make_async_copy(key_hbm.at[pl.ds(2 * p, 2)], kbuf.at[pl.ds(2 * p, 2)], ksem.at[p])

    def value_copy(p):
        return pltpu.make_async_copy(value_hbm.at[pl.ds(2 * p, 2)], vbuf.at[pl.ds(2 * p, 2)], vsem.at[p])

    first_copies = (
        (wq_hbm, wq),
        (wk_hbm, wk),
        (wv_hbm, wv),
        (wo_hbm, wo),
        (tokens_hbm, tokens),
        (gain_hbm, gain),
        (lengths_hbm, lengths),
        (offsets_hbm, offsets),
    )
    weights = [pltpu.make_async_copy(src, dst, wsem.at[i]) for i, (src, dst) in enumerate(first_copies)]
    for copy in weights[4:] + weights[:3]:
        copy.start()
    for p in range(pairs):
        key_copy(p).start()
        value_copy(p).start()
    weights[3].start()

    for copy in weights[4:]:
        copy.wait()
    normed = rms_rows(tokens[...], gain[...])
    weights[0].wait()
    queries = dot(normed, wq[...]).astype(bf16).astype(f32)
    lane = iota((seqs, LANES), 1)
    for h in range(heads):
        tile = queries[:, (h // 2) * LANES : (h // 2 + 1) * LANES]
        upper = h >= heads // 2
        if (h % 2 == 1) != upper:
            tile = pltpu.roll(tile, HEAD_DIM, 1)
        tile = jnp.where((lane >= HEAD_DIM) == upper, tile, 0.0)
        qrows[pl.ds(h, seqs, stride=heads), :] = tile
    weights[1].wait()
    keys_out[...] = dot(normed, wk[...]).astype(bf16)
    weights[2].wait()
    values_out[...] = dot(normed, wv[...]).astype(bf16)

    rows = 2 * heads
    head_of = iota((rows, LANES), 0) % heads
    offset = jnp.zeros((rows, LANES), f32)
    for h in range(heads):
        offset = jnp.where(head_of == h, offsets[h], offset)
    first = iota((rows, LANES), 0) < heads
    tri_row = iota((2 * LANES, 2 * LANES), 0) % LANES
    tri_col = iota((2 * LANES, 2 * LANES), 1)
    later = jnp.where((tri_row > tri_col) | (tri_col >= LANES), 1.0, 0.0).astype(bf16)
    position = iota((rows, LANES), 1)
    zero = jnp.zeros((heads, LANES), f32)

    def one_pair(p, carry):
        key_copy(p).wait()
        base = pl.multiple_of(p * rows, rows)
        both = qrows[pl.ds(base, rows), :]
        left = jnp.concatenate([both[:heads], zero], axis=0)
        right = jnp.concatenate([zero, both[heads:]], axis=0)
        query = jnp.concatenate([left, right], axis=1).astype(bf16)
        keys = jnp.concatenate([kbuf[2 * p], kbuf[2 * p + 1]], axis=1)
        scores = dot(query, keys, ((1,), (1,)))
        limit = jnp.where(first, lengths[2 * p], lengths[2 * p + 1])
        taken = []
        highs = []
        lows = []
        for c in range(blocks):
            z = scores[:, c * LANES : (c + 1) * LANES] * HEAD_DIM ** (-0.5) + offset
            tail = jnp.log1p(jnp.exp(-jnp.abs(z)))
            fail = jnp.where(position + c * LANES < limit, -(jnp.maximum(z, 0.0) + tail), 0.0)
            taken.append(jnp.minimum(z, 0.0) - tail)
            high, low = split_two(fail)
            highs.append(high)
            lows.append(low)
        halves = jnp.concatenate([jnp.concatenate(highs, axis=0), jnp.concatenate(lows, axis=0)], axis=1)
        sums = dot(halves, later)
        carried = jnp.zeros((rows, LANES), f32)
        sticks = [None] * blocks
        for c in reversed(range(blocks)):
            block = sums[c * rows : (c + 1) * rows]
            share = jnp.exp(taken[c] + (block[:, :LANES] + carried))
            sticks[c] = jnp.where(position + c * LANES < limit, share, 0.0).astype(bf16)
            carried = carried + block[:, LANES:]
        stick = jnp.concatenate(sticks, axis=1)
        value_copy(p).wait()
        values = jnp.concatenate([vbuf[2 * p], vbuf[2 * p + 1]], axis=1)
        attended = dot(stick, values)
        arows[pl.ds(base, rows), :] = jnp.where(first, attended[:, :LANES], attended[:, LANES:])
        return carry

    lax.fori_loop(0, pairs, one_pair, 0)

    tiles = []
    for q in range(heads // 2):
        upper = 2 * q >= heads // 2
        even = arows[pl.ds(2 * q, seqs, stride=heads), :]
        odd = arows[pl.ds(2 * q + 1, seqs, stride=heads), :]
        if upper:
            even = pltpu.roll(even, HEAD_DIM, 1)
        else:
            odd = pltpu.roll(odd, HEAD_DIM, 1)
        tiles.append(jnp.where(lane < HEAD_DIM, even, odd))
    attended = jnp.concatenate(tiles, axis=1).astype(bf16)
    weights[3].wait()
    part_out[...] = dot(attended, wo[...]).astype(bf16)


def attention(lengths, offsets, tokens, gain, key_cache, value_cache, w_query, w_key, w_value, w_out):
    seqs, width = tokens.shape
    heads = offsets.shape[0]
    kv = w_key.shape[1]
    vmem = pl.BlockSpec(memory_space=pltpu.VMEM)
    hbm = pl.BlockSpec(memory_space=pltpu.HBM)
    caches = [
        pltpu.with_memory_space_constraint(x, pltpu.HBM)
        for x in (lengths, offsets, tokens, gain, key_cache, value_cache, w_query, w_key, w_value, w_out)
    ]
    return pl.pallas_call(
        attention_kernel,
        out_shape=(
            jax.ShapeDtypeStruct((seqs, width), bf16),
            jax.ShapeDtypeStruct((seqs, kv), bf16),
            jax.ShapeDtypeStruct((seqs, kv), bf16),
        ),
        in_specs=[hbm] * 10,
        out_specs=(vmem, vmem, vmem),
        scratch_shapes=[
            pltpu.SMEM(lengths.shape, jnp.int32),
            pltpu.SMEM(offsets.shape, f32),
            pltpu.VMEM(tokens.shape, bf16),
            pltpu.VMEM(gain.shape, f32),
            pltpu.VMEM(key_cache.shape, bf16),
            pltpu.VMEM(value_cache.shape, bf16),
            pltpu.VMEM(w_query.shape, bf16),
            pltpu.VMEM(w_key.shape, bf16),
            pltpu.VMEM(w_value.shape, bf16),
            pltpu.VMEM(w_out.shape, bf16),
            pltpu.VMEM((seqs * heads, LANES), f32),
            pltpu.VMEM((seqs * heads, LANES), f32),
            pltpu.SemaphoreType.DMA((8,)),
            pltpu.SemaphoreType.DMA((seqs // 2,)),
            pltpu.SemaphoreType.DMA((seqs // 2,)),
        ],
        compiler_params=pltpu.CompilerParams(vmem_limit_bytes=32 << 20),
        name="attention",
    )(*caches)


def dispatch_kernel(
    tokens, gain, own, peer, routes_hbm, weights_hbm, rows_out, middle_out, mix_out, route, weight, sems
):
    seqs, width = tokens.shape
    slots, half = rows_out.shape
    capacity = slots // EXPERTS
    start = lax.axis_index("ep") * seqs
    tile = pl.multiple_of(start // LANES * LANES, LANES)
    copies = [
        pltpu.make_async_copy(routes_hbm.at[:, pl.ds(tile, LANES)], route, sems.at[0]),
        pltpu.make_async_copy(weights_hbm.at[:, pl.ds(tile, LANES)], weight, sems.at[1]),
    ]
    for copy in copies:
        copy.start()
    low_half = lax.axis_index("tp") == 0
    middle = (tokens[...].astype(f32) + own[...].astype(f32) + peer[...].astype(f32)).astype(bf16)
    moe_in = rms_rows(middle, gain[...]).astype(f32)
    mine = jnp.where(low_half, moe_in[:, :half], moe_in[:, half:]).astype(bf16)
    middle = middle.astype(f32)
    middle_out[...] = jnp.where(low_half, middle[:, :half], middle[:, half:]).astype(bf16)
    for copy in copies:
        copy.wait()
    here = iota((seqs, LANES), 1) == iota((seqs, LANES), 0) + (start - tile)

    def column(values):
        return jnp.sum(jnp.where(here, values, 0.0), axis=1, keepdims=True)

    r0, r1 = (column(route[i : i + 1, :].astype(f32)) for i in range(2))
    w0, w1 = (column(weight[i : i + 1, :]) for i in range(2))
    earlier = jnp.where(iota((seqs, seqs), 1) < iota((seqs, seqs), 0), 1.0, 0.0).astype(bf16)

    def slot_mask(expert, slot):
        expert = expert.astype(f32)
        first = r0 == expert
        named = first | (r1 == expert)
        before = dot(earlier, jnp.where(named, 1.0, 0.0).astype(bf16))
        return first, named & (before == slot.astype(f32))

    index = iota((seqs, slots), 1)
    _, chosen = slot_mask(index // capacity, index % capacity)
    rows_out[...] = dot(jnp.where(chosen, 1.0, 0.0).astype(bf16), mine, ((0,), (0,))).astype(bf16)
    returned = mix_out.shape[1]
    index = iota((seqs, returned), 1)
    first, chosen = slot_mask(index // (returned // EXPERTS), index % capacity)
    high, low = split_two(jnp.where(chosen, jnp.where(first, w0, w1), 0.0))
    mix_out[...] = jnp.concatenate([high, low], axis=0)


def dispatch(tokens, gain, own, peer, routes, weights, capacity, sources):
    seqs, width = tokens.shape
    vmem = pl.BlockSpec(memory_space=pltpu.VMEM)
    hbm = pl.BlockSpec(memory_space=pltpu.HBM)
    outs = ((EXPERTS * capacity, width // 2), (seqs, width // 2), (2 * seqs, sources * capacity))
    return pl.pallas_call(
        dispatch_kernel,
        out_shape=tuple(jax.ShapeDtypeStruct(shape, bf16) for shape in outs),
        in_specs=[vmem] * 4 + [hbm] * 2,
        out_specs=(vmem,) * 3,
        scratch_shapes=[
            pltpu.VMEM((2, LANES), jnp.int32),
            pltpu.VMEM((2, LANES), f32),
            pltpu.SemaphoreType.DMA((2,)),
        ],
        compiler_params=pltpu.CompilerParams(vmem_limit_bytes=8 << 20),
        name="dispatch",
    )(tokens, gain, own, peer, routes, weights)


def expert_kernel(own, peer, gate_w, up_w, down_w, keep_out, send_out):
    half = own.shape[1]
    tp_index = lax.axis_index("tp")
    mine = pl.multiple_of(tp_index * half, half)
    other = pl.multiple_of((1 - tp_index) * half, half)
    x, y = own[...], peer[...]

    def project(w):
        return dot(x, w[:, pl.ds(mine, half)], ((1,), (1,))) + dot(y, w[:, pl.ds(other, half)], ((1,), (1,)))

    gate = project(gate_w)
    upward = project(up_w)
    hidden = (gate / (1.0 + jnp.exp(-gate)) * upward).astype(bf16)
    send_out[...] = dot(hidden, down_w[:, pl.ds(other, half)]).astype(bf16)
    keep_out[...] = dot(hidden, down_w[:, pl.ds(mine, half)])


def expert(own, peer, gate_w, up_w, down_w):
    vmem = pl.BlockSpec(memory_space=pltpu.VMEM)
    return pl.pallas_call(
        expert_kernel,
        out_shape=(jax.ShapeDtypeStruct(own.shape, f32), jax.ShapeDtypeStruct(own.shape, bf16)),
        in_specs=[vmem] * 5,
        out_specs=(vmem, vmem),
        compiler_params=pltpu.CompilerParams(vmem_limit_bytes=32 << 20),
        name="expert",
    )(own, peer, gate_w, up_w, down_w)


def mix_kernel(mix, returned, middle, out):
    seqs = middle.shape[0]
    both = dot(mix[...], returned[...])
    out[...] = (middle[...].astype(f32) + (both[:seqs] + both[seqs:])).astype(bf16)


def mix_rows(mix, returned, middle):
    vmem = pl.BlockSpec(memory_space=pltpu.VMEM)
    return pl.pallas_call(
        mix_kernel,
        out_shape=jax.ShapeDtypeStruct(middle.shape, bf16),
        in_specs=[vmem] * 3,
        out_specs=vmem,
        compiler_params=pltpu.CompilerParams(vmem_limit_bytes=8 << 20),
        name="mix",
    )(mix, returned, middle)


def shards(
    tokens,
    lengths,
    routes,
    route_weights,
    key_cache,
    value_cache,
    w_query,
    w_key,
    w_value,
    w_out,
    score_offset,
    attn_gain,
    ffn_gain,
    w_gate,
    w_up,
    w_down,
):
    seqs, width = tokens.shape
    sources = lax.axis_size("ep")
    span = sources // EXPERTS
    capacity = 4
    half = width // 2
    swap = [(0, 1), (1, 0)]
    part, new_keys, new_values = attention(
        lengths,
        score_offset,
        tokens,
        attn_gain.reshape(1, width),
        key_cache,
        value_cache,
        w_query,
        w_key,
        w_value,
        w_out,
    )
    other_part = lax.ppermute(part, "tp", swap)
    rows, middle, mix = dispatch(
        tokens,
        ffn_gain.reshape(1, width),
        part,
        other_part,
        routes.T,
        route_weights.T,
        capacity,
        sources,
    )
    outgoing = jnp.broadcast_to(
        rows.reshape(EXPERTS, 1, capacity, half), (EXPERTS, span, capacity, half)
    ).reshape(sources, capacity, half)
    arrived = lax.all_to_all(outgoing, "ep", split_axis=0, concat_axis=0, tiled=True)
    own = arrived.reshape(sources * capacity, half)
    peer = lax.ppermute(own, "tp", swap)
    keep, send = expert(own, peer, w_gate.T, w_up.T, w_down)
    got = lax.ppermute(send, "tp", swap)
    shares = (keep + got.astype(f32)).astype(bf16).reshape(sources, capacity, half)
    returned = lax.all_to_all(shares, "ep", split_axis=0, concat_axis=0, tiled=True)
    layer_out = mix_rows(mix, returned.reshape(sources * capacity, half), middle)
    return (layer_out, new_keys, new_values)


def solution(mesh):
    in_specs = (
        P("ep", None),
        P("ep"),
        P(),
        P(),
        P("ep", None, "tp"),
        P("ep", None, "tp"),
        P(None, "tp"),
        P(None, "tp"),
        P(None, "tp"),
        P("tp", None),
        P("tp"),
        P(),
        P(),
        P(None, ("ep", "tp")),
        P(None, ("ep", "tp")),
        P(("ep", "tp"), None),
    )
    out_specs = (P("ep", "tp"), P("ep", "tp"), P("ep", "tp"))
    return jax.shard_map(shards, mesh=mesh, in_specs=in_specs, out_specs=out_specs, check_vma=False)
```

```python
import jax
import jax.numpy as jnp
from jax import lax
from jax.experimental import pallas as pl
from jax.experimental.pallas import tpu as pltpu
from jax.sharding import PartitionSpec as P

HEAD_DIM = 64
EXPERTS = 16
LANES = 128
GROUPS = (4, 4)
PLANES = 8
norm_eps = 1e-06

f32 = jnp.float32
bf16 = jnp.bfloat16


def rms_rows(values, gain_row):
    widened = values.astype(f32)
    scaled = widened * lax.rsqrt(jnp.mean(widened * widened, axis=-1, keepdims=True) + norm_eps)
    return (scaled * gain_row).astype(bf16)


def dot(a, b, dims=((1,), (0,))):
    return lax.dot_general(a, b, (dims, ((), ())), preferred_element_type=f32)


def split_two(x):
    high = x.astype(bf16)
    return high, (x - high.astype(f32)).astype(bf16)


def iota(shape, dim):
    return lax.broadcasted_iota(jnp.int32, shape, dim)


def attention_kernel(
    lengths_hbm,
    offsets_hbm,
    tokens_hbm,
    gain_hbm,
    key_hbm,
    value_hbm,
    wq_hbm,
    wk_hbm,
    wv_hbm,
    wo_hbm,
    part_out,
    keys_hbm,
    values_hbm,
    lengths,
    offsets,
    tokens,
    gain,
    kbuf,
    vbuf,
    wq,
    wk,
    wv,
    wo,
    qrows,
    arows,
    later,
    new_keys,
    new_values,
    wsem,
    ksem,
    vsem,
    osem,
):
    seqs, context, width = kbuf.shape
    heads = qrows.shape[0] // seqs
    pairs = seqs // 2
    blocks = context // LANES

    def key_copy(p):
        return pltpu.make_async_copy(key_hbm.at[pl.ds(2 * p, 2)], kbuf.at[pl.ds(2 * p, 2)], ksem.at[p])

    def value_copy(p):
        return pltpu.make_async_copy(value_hbm.at[pl.ds(2 * p, 2)], vbuf.at[pl.ds(2 * p, 2)], vsem.at[p])

    first_copies = (
        (wq_hbm, wq),
        (wk_hbm, wk),
        (wv_hbm, wv),
        (wo_hbm, wo),
        (tokens_hbm, tokens),
        (gain_hbm, gain),
        (lengths_hbm, lengths),
        (offsets_hbm, offsets),
    )
    weights = [pltpu.make_async_copy(src, dst, wsem.at[i]) for i, (src, dst) in enumerate(first_copies)]
    for copy in weights[4:] + weights[:3]:
        copy.start()
    for copy in weights[4:]:
        copy.wait()
    groups = [range(sum(GROUPS[:i]), sum(GROUPS[: i + 1])) for i in range(len(GROUPS))]
    for members in groups:
        if members is groups[-1]:
            weights[3].start()
        for p in members:
            key_copy(p).start()
        for p in members:
            value_copy(p).start()

    normed = rms_rows(tokens[...], gain[...])
    for copy in weights[:3]:
        copy.wait()
    queries = dot(normed, wq[...]).astype(bf16).astype(f32)
    new_keys[...] = dot(normed, wk[...]).astype(bf16)
    new_values[...] = dot(normed, wv[...]).astype(bf16)
    lane = iota((seqs, LANES), 1)
    for h in range(heads):
        tile = queries[:, (h // 2) * LANES : (h // 2 + 1) * LANES]
        upper = h >= heads // 2
        if (h % 2 == 1) != upper:
            tile = pltpu.roll(tile, HEAD_DIM, 1)
        tile = jnp.where((lane >= HEAD_DIM) == upper, tile, 0.0)
        qrows[pl.ds(h, seqs, stride=heads), :] = tile
    outs = [
        pltpu.make_async_copy(new_keys, keys_hbm, osem.at[0]),
        pltpu.make_async_copy(new_values, values_hbm, osem.at[1]),
    ]
    for copy in outs:
        copy.start()

    rows = 2 * heads
    head_of = iota((rows, LANES), 0) % heads
    offset = jnp.zeros((rows, LANES), f32)
    for h in range(heads):
        offset = jnp.where(head_of == h, offsets[h], offset)
    first = iota((rows, LANES), 0) < heads
    tri_row = iota((2 * LANES, 2 * LANES), 0) % LANES
    tri_col = iota((2 * LANES, 2 * LANES), 1)
    later[...] = jnp.where((tri_row > tri_col) | (tri_col >= LANES), 1.0, 0.0).astype(bf16)
    position = iota((rows, LANES), 1)
    zero = jnp.zeros((heads, LANES), f32)

    def one_group(members):
        limits = [jnp.where(first, lengths[2 * p], lengths[2 * p + 1]) for p in members]
        for p in members:
            key_copy(p).wait()
        scores = []
        for p in members:
            both = qrows[p * rows : (p + 1) * rows, :]
            left = jnp.concatenate([both[:heads], zero], axis=0)
            right = jnp.concatenate([zero, both[heads:]], axis=0)
            query = jnp.concatenate([left, right], axis=1).astype(bf16)
            keys = jnp.concatenate([kbuf[2 * p], kbuf[2 * p + 1]], axis=1)
            scores.append(dot(query, keys, ((1,), (1,))))
        taken = {}
        highs = []
        lows = []
        for i in range(len(members)):
            for c in range(blocks):
                z = scores[i][:, c * LANES : (c + 1) * LANES] * HEAD_DIM ** (-0.5) + offset
                tail = jnp.log1p(jnp.exp(-jnp.abs(z)))
                fail = jnp.where(position + c * LANES < limits[i], -(jnp.maximum(z, 0.0) + tail), 0.0)
                taken[i, c] = jnp.minimum(z, 0.0) - tail
                high, low = split_two(fail)
                highs.append(high)
                lows.append(low)
        halves = jnp.concatenate([jnp.concatenate(highs, axis=0), jnp.concatenate(lows, axis=0)], axis=1)
        sums = dot(halves, later[...])
        sticks = []
        for i in range(len(members)):
            carried = jnp.zeros((rows, LANES), f32)
            stick = [None] * blocks
            for c in reversed(range(blocks)):
                at = (i * blocks + c) * rows
                share = jnp.exp(taken[i, c] + (sums[at : at + rows, :LANES] + carried))
                stick[c] = jnp.where(position + c * LANES < limits[i], share, 0.0).astype(bf16)
                carried = carried + sums[at : at + rows, LANES:]
            sticks.append(jnp.concatenate(stick, axis=1))
        for p in members:
            value_copy(p).wait()
        for i, p in enumerate(members):
            values = jnp.concatenate([vbuf[2 * p], vbuf[2 * p + 1]], axis=1)
            attended = dot(sticks[i], values)
            arows[p * rows : (p + 1) * rows, :] = jnp.where(first, attended[:, :LANES], attended[:, LANES:])

    for members in groups:
        one_group(members)

    tiles = []
    for q in range(heads // 2):
        upper = 2 * q >= heads // 2
        even = arows[pl.ds(2 * q, seqs, stride=heads), :]
        odd = arows[pl.ds(2 * q + 1, seqs, stride=heads), :]
        if upper:
            even = pltpu.roll(even, HEAD_DIM, 1)
        else:
            odd = pltpu.roll(odd, HEAD_DIM, 1)
        tiles.append(jnp.where(lane < HEAD_DIM, even, odd))
    attended = jnp.concatenate(tiles, axis=1).astype(bf16)
    weights[3].wait()
    part_out[...] = dot(attended, wo[...]).astype(bf16)
    for copy in outs:
        copy.wait()


def attention(lengths, offsets, tokens, gain, key_cache, value_cache, w_query, w_key, w_value, w_out):
    seqs, width = tokens.shape
    heads = offsets.shape[0]
    kv = w_key.shape[1]
    vmem = pl.BlockSpec(memory_space=pltpu.VMEM)
    hbm = pl.BlockSpec(memory_space=pltpu.HBM)
    caches = [
        pltpu.with_memory_space_constraint(x, pltpu.HBM)
        for x in (lengths, offsets, tokens, gain, key_cache, value_cache, w_query, w_key, w_value, w_out)
    ]
    return pl.pallas_call(
        attention_kernel,
        out_shape=(
            jax.ShapeDtypeStruct((seqs, width), bf16),
            jax.ShapeDtypeStruct((seqs, kv), bf16),
            jax.ShapeDtypeStruct((seqs, kv), bf16),
        ),
        in_specs=[hbm] * 10,
        out_specs=(vmem, hbm, hbm),
        scratch_shapes=[
            pltpu.SMEM(lengths.shape, jnp.int32),
            pltpu.SMEM(offsets.shape, f32),
            pltpu.VMEM(tokens.shape, bf16),
            pltpu.VMEM(gain.shape, f32),
            pltpu.VMEM(key_cache.shape, bf16),
            pltpu.VMEM(value_cache.shape, bf16),
            pltpu.VMEM(w_query.shape, bf16),
            pltpu.VMEM(w_key.shape, bf16),
            pltpu.VMEM(w_value.shape, bf16),
            pltpu.VMEM(w_out.shape, bf16),
            pltpu.VMEM((seqs * heads, LANES), f32),
            pltpu.VMEM((seqs * heads, LANES), f32),
            pltpu.VMEM((2 * LANES, 2 * LANES), bf16),
            pltpu.VMEM((seqs, kv), bf16),
            pltpu.VMEM((seqs, kv), bf16),
            pltpu.SemaphoreType.DMA((8,)),
            pltpu.SemaphoreType.DMA((seqs // 2,)),
            pltpu.SemaphoreType.DMA((seqs // 2,)),
            pltpu.SemaphoreType.DMA((2,)),
        ],
        compiler_params=pltpu.CompilerParams(vmem_limit_bytes=20 << 20),
        name="attention",
    )(*caches)


def dispatch_kernel(
    tokens, gain, own, peer, routes_hbm, weights_hbm, rows_out, middle_out, mix_out, route, weight, sems
):
    seqs, width = tokens.shape
    slots, half = rows_out.shape
    capacity = slots // EXPERTS
    start = lax.axis_index("ep") * seqs
    tile = pl.multiple_of(start // LANES * LANES, LANES)
    copies = [
        pltpu.make_async_copy(routes_hbm.at[:, pl.ds(tile, LANES)], route, sems.at[0]),
        pltpu.make_async_copy(weights_hbm.at[:, pl.ds(tile, LANES)], weight, sems.at[1]),
    ]
    for copy in copies:
        copy.start()
    low_half = lax.axis_index("tp") == 0
    middle = (tokens[...].astype(f32) + own[...].astype(f32) + peer[...].astype(f32)).astype(bf16)
    moe_in = rms_rows(middle, gain[...]).astype(f32)
    mine = jnp.where(low_half, moe_in[:, :half], moe_in[:, half:]).astype(bf16)
    middle = middle.astype(f32)
    middle_out[...] = jnp.where(low_half, middle[:, :half], middle[:, half:]).astype(bf16)
    for copy in copies:
        copy.wait()
    here = iota((seqs, LANES), 1) == iota((seqs, LANES), 0) + (start - tile)

    def column(values):
        return jnp.sum(jnp.where(here, values, 0.0), axis=1, keepdims=True)

    r0, r1 = (column(route[i : i + 1, :].astype(f32)) for i in range(2))
    w0, w1 = (column(weight[i : i + 1, :]) for i in range(2))
    earlier = jnp.where(iota((seqs, seqs), 1) < iota((seqs, seqs), 0), 1.0, 0.0).astype(bf16)

    def slot_mask(expert, slot):
        expert = expert.astype(f32)
        first = r0 == expert
        named = first | (r1 == expert)
        before = dot(earlier, jnp.where(named, 1.0, 0.0).astype(bf16))
        return first, named & (before == slot.astype(f32))

    index = iota((seqs, slots), 1)
    first, chosen = slot_mask(index // capacity, index % capacity)
    rows_out[...] = dot(jnp.where(chosen, 1.0, 0.0).astype(bf16), mine, ((0,), (0,))).astype(bf16)
    high, low = split_two(jnp.where(chosen, jnp.where(first, w0, w1), 0.0))
    mix_out[...] = jnp.concatenate([high, low], axis=0)


def dispatch(tokens, gain, own, peer, routes, weights, capacity):
    seqs, width = tokens.shape
    vmem = pl.BlockSpec(memory_space=pltpu.VMEM)
    hbm = pl.BlockSpec(memory_space=pltpu.HBM)
    outs = ((EXPERTS * capacity, width // 2), (seqs, width // 2), (2 * seqs, EXPERTS * capacity))
    return pl.pallas_call(
        dispatch_kernel,
        out_shape=tuple(jax.ShapeDtypeStruct(shape, bf16) for shape in outs),
        in_specs=[vmem] * 4 + [hbm] * 2,
        out_specs=(vmem,) * 3,
        scratch_shapes=[
            pltpu.VMEM((2, LANES), jnp.int32),
            pltpu.VMEM((2, LANES), f32),
            pltpu.SemaphoreType.DMA((2,)),
        ],
        compiler_params=pltpu.CompilerParams(vmem_limit_bytes=8 << 20),
        name="dispatch",
    )(tokens, gain, own, peer, routes, weights)


def own_columns(half):
    tp_index = lax.axis_index("tp")
    return pl.multiple_of(tp_index * half, half), pl.multiple_of((1 - tp_index) * half, half)


def enter_kernel(own, gate_w, up_w, down_hbm, gate_out, up_out, down_out, sem):
    half = own.shape[1]
    mine, _ = own_columns(half)
    copy = pltpu.make_async_copy(down_hbm, down_out, sem)
    copy.start()
    gate_out[...] = dot(own[...], gate_w[:, pl.ds(mine, half)], ((1,), (1,)))
    up_out[...] = dot(own[...], up_w[:, pl.ds(mine, half)], ((1,), (1,)))
    copy.wait()


def hidden_kernel(peer, gate_part, up_part, gate_w, up_w, down_w, hidden_out, send_out):
    half = peer.shape[1]
    _, other = own_columns(half)
    gate = gate_part[...] + dot(peer[...], gate_w[:, pl.ds(other, half)], ((1,), (1,)))
    upward = up_part[...] + dot(peer[...], up_w[:, pl.ds(other, half)], ((1,), (1,)))
    hidden = (gate / (1.0 + jnp.exp(-gate)) * upward).astype(bf16)
    hidden_out[...] = hidden
    send_out[...] = dot(hidden, down_w[:, pl.ds(other, half)]).astype(bf16)


def keep_kernel(hidden, down_w, keep_out):
    half = keep_out.shape[1]
    mine, _ = own_columns(half)
    keep_out[...] = dot(hidden[...], down_w[:, pl.ds(mine, half)])


def local_call(kernel, outs, *args, far=0):
    vmem = pl.BlockSpec(memory_space=pltpu.VMEM)
    hbm = pl.BlockSpec(memory_space=pltpu.HBM)
    rows, half = args[0].shape
    near = len(args) - far
    args = args[:near] + tuple(pltpu.with_memory_space_constraint(x, pltpu.HBM) for x in args[near:])
    return pl.pallas_call(
        kernel,
        out_shape=tuple(jax.ShapeDtypeStruct(shape, kind) for shape, kind in outs),
        in_specs=[vmem] * near + [hbm] * far,
        out_specs=(vmem,) * len(outs),
        scratch_shapes=[pltpu.SemaphoreType.DMA(())] * far,
        compiler_params=pltpu.CompilerParams(vmem_limit_bytes=12 << 20),
        cost_estimate=pl.CostEstimate(flops=2 * rows * half * half, transcendentals=0, bytes_accessed=rows * half * 4),
        name=kernel.__name__[:-7],
    )(*args)


def mix_kernel(mix, returned, middle, out):
    seqs = middle.shape[0]
    both = dot(mix[...], returned[...])
    out[...] = (middle[...].astype(f32) + (both[:seqs] + both[seqs:])).astype(bf16)


def mix_rows(mix, returned, middle):
    vmem = pl.BlockSpec(memory_space=pltpu.VMEM)
    return pl.pallas_call(
        mix_kernel,
        out_shape=jax.ShapeDtypeStruct(middle.shape, bf16),
        in_specs=[vmem] * 3,
        out_specs=vmem,
        compiler_params=pltpu.CompilerParams(vmem_limit_bytes=8 << 20),
        name="mix",
    )(mix, returned, middle)


def shards(
    tokens,
    lengths,
    routes,
    route_weights,
    key_cache,
    value_cache,
    w_query,
    w_key,
    w_value,
    w_out,
    score_offset,
    attn_gain,
    ffn_gain,
    w_gate,
    w_up,
    w_down,
):
    seqs, width = tokens.shape
    sources = lax.axis_size("ep")
    capacity = 4
    half = width // 2
    swap = [(0, 1), (1, 0)]
    part, new_keys, new_values = attention(
        lengths,
        score_offset,
        tokens,
        attn_gain.reshape(1, width),
        key_cache,
        value_cache,
        w_query,
        w_key,
        w_value,
        w_out,
    )
    other_part = lax.ppermute(part, "tp", swap)
    rows, middle, mix = dispatch(
        tokens,
        ffn_gain.reshape(1, width),
        part,
        other_part,
        routes.T,
        route_weights.T,
        capacity,
    )
    plane = sources // PLANES
    sides = EXPERTS // PLANES
    column_groups = [[p * plane + c for p in range(PLANES)] for c in range(plane)]
    plane_groups = [[p * plane + c for c in range(plane)] for p in range(PLANES)]

    def exchange(x, groups):
        return lax.all_to_all(x, "ep", 0, 0, axis_index_groups=groups, tiled=True)

    landed = exchange(rows.reshape(PLANES, sides * capacity, half), column_groups)
    landed = landed.reshape(PLANES, sides, capacity, half).transpose(1, 0, 2, 3)
    outgoing = jnp.broadcast_to(landed[:, None], (sides, plane // sides) + landed.shape[1:])
    arrived = exchange(outgoing.reshape((plane,) + landed.shape[1:]), plane_groups)
    own = arrived.reshape(sources * capacity, half)
    peer = lax.ppermute(own, "tp", swap)
    gate_w, up_w = w_gate.T, w_up.T
    inner = (own.shape[0], gate_w.shape[0])
    *parts, down_w = local_call(
        enter_kernel, ((inner, f32), (inner, f32), (w_down.shape, bf16)), own, gate_w, up_w, w_down, far=1
    )
    hidden, send = local_call(
        hidden_kernel, ((inner, bf16), (own.shape, bf16)), peer, *parts, gate_w, up_w, down_w
    )
    got = lax.ppermute(send, "tp", swap)
    (keep,) = local_call(keep_kernel, ((own.shape, f32),), hidden, down_w)
    shares = (keep + got.astype(f32)).astype(bf16).reshape(plane, PLANES, capacity, half)
    landed = exchange(shares, plane_groups)
    landed = landed.reshape(sides, plane // sides, PLANES, capacity, half).astype(f32).sum(axis=1)
    landed = landed.astype(bf16).transpose(1, 0, 2, 3).reshape(PLANES, sides * capacity, half)
    returned = exchange(landed, column_groups)
    layer_out = mix_rows(mix, returned.reshape(EXPERTS * capacity, half), middle)
    return (layer_out, new_keys, new_values)


def solution(mesh):
    in_specs = (
        P("ep", None),
        P("ep"),
        P(),
        P(),
        P("ep", None, "tp"),
        P("ep", None, "tp"),
        P(None, "tp"),
        P(None, "tp"),
        P(None, "tp"),
        P("tp", None),
        P("tp"),
        P(),
        P(),
        P(None, ("ep", "tp")),
        P(None, ("ep", "tp")),
        P(("ep", "tp"), None),
    )
    out_specs = (P("ep", "tp"), P("ep", "tp"), P("ep", "tp"))
    return jax.shard_map(shards, mesh=mesh, in_specs=in_specs, out_specs=out_specs, check_vma=False)
```

```python
import jax
import jax.numpy as jnp
from jax import lax
from jax.experimental import pallas as pl
from jax.experimental.pallas import tpu as pltpu
from jax.sharding import Mesh
from jax.sharding import PartitionSpec as P

HEAD_DIM = 64
EXPERTS = 16
LANES = 128
GROUPS = (4, 4)
PLANES = 8
SIDES = EXPERTS // PLANES
norm_eps = 1e-06

f32 = jnp.float32
bf16 = jnp.bfloat16


def rms_rows(values, gain_row):
    widened = values.astype(f32)
    scaled = widened * lax.rsqrt(jnp.mean(widened * widened, axis=-1, keepdims=True) + norm_eps)
    return (scaled * gain_row).astype(bf16)


def dot(a, b, dims=((1,), (0,))):
    return lax.dot_general(a, b, (dims, ((), ())), preferred_element_type=f32)


def split_two(x):
    high = x.astype(bf16)
    return high, (x - high.astype(f32)).astype(bf16)


def iota(shape, dim):
    return lax.broadcasted_iota(jnp.int32, shape, dim)


def attention_kernel(
    lengths_hbm,
    offsets_hbm,
    tokens_hbm,
    gain_hbm,
    key_hbm,
    value_hbm,
    wq_hbm,
    wk_hbm,
    wv_hbm,
    wo_hbm,
    part_out,
    keys_hbm,
    values_hbm,
    lengths,
    offsets,
    tokens,
    gain,
    kbuf,
    vbuf,
    wq,
    wk,
    wv,
    wo,
    qrows,
    arows,
    later,
    new_keys,
    new_values,
    wsem,
    ksem,
    vsem,
    osem,
):
    seqs, context, _ = kbuf.shape
    heads = qrows.shape[0] // seqs
    blocks = context // LANES

    def key_copy(p):
        return pltpu.make_async_copy(key_hbm.at[pl.ds(2 * p, 2)], kbuf.at[pl.ds(2 * p, 2)], ksem.at[p])

    def value_copy(p):
        return pltpu.make_async_copy(value_hbm.at[pl.ds(2 * p, 2)], vbuf.at[pl.ds(2 * p, 2)], vsem.at[p])

    first_copies = (
        (wq_hbm, wq),
        (wk_hbm, wk),
        (wv_hbm, wv),
        (wo_hbm, wo),
        (tokens_hbm, tokens),
        (gain_hbm, gain),
        (lengths_hbm, lengths),
        (offsets_hbm, offsets),
    )
    weights = [pltpu.make_async_copy(src, dst, wsem.at[i]) for i, (src, dst) in enumerate(first_copies)]
    for copy in weights[4:] + weights[:3]:
        copy.start()
    for copy in weights[4:]:
        copy.wait()
    groups = [range(sum(GROUPS[:i]), sum(GROUPS[: i + 1])) for i in range(len(GROUPS))]
    for members in groups:
        if members is groups[-1]:
            weights[3].start()
        for p in members:
            key_copy(p).start()
        for p in members:
            value_copy(p).start()

    normed = rms_rows(tokens[...], gain[...])
    for copy in weights[:3]:
        copy.wait()
    queries = dot(normed, wq[...]).astype(bf16).astype(f32)
    new_keys[...] = dot(normed, wk[...]).astype(bf16)
    new_values[...] = dot(normed, wv[...]).astype(bf16)
    lane = iota((seqs, LANES), 1)
    for h in range(heads):
        tile = queries[:, (h // 2) * LANES : (h // 2 + 1) * LANES]
        upper = h >= heads // 2
        if (h % 2 == 1) != upper:
            tile = pltpu.roll(tile, HEAD_DIM, 1)
        tile = jnp.where((lane >= HEAD_DIM) == upper, tile, 0.0)
        qrows[pl.ds(h, seqs, stride=heads), :] = tile
    outs = [
        pltpu.make_async_copy(new_keys, keys_hbm, osem.at[0]),
        pltpu.make_async_copy(new_values, values_hbm, osem.at[1]),
    ]
    for copy in outs:
        copy.start()

    rows = 2 * heads
    head_of = iota((rows, LANES), 0) % heads
    offset = jnp.zeros((rows, LANES), f32)
    for h in range(heads):
        offset = jnp.where(head_of == h, offsets[h], offset)
    first = iota((rows, LANES), 0) < heads
    tri_row = iota((2 * LANES, 2 * LANES), 0) % LANES
    tri_col = iota((2 * LANES, 2 * LANES), 1)
    later[...] = jnp.where((tri_row > tri_col) | (tri_col >= LANES), 1.0, 0.0).astype(bf16)
    position = iota((rows, LANES), 1)
    zero = jnp.zeros((heads, LANES), f32)

    def one_group(members):
        limits = [jnp.where(first, lengths[2 * p], lengths[2 * p + 1]) for p in members]
        for p in members:
            key_copy(p).wait()
        scores = []
        for p in members:
            both = qrows[p * rows : (p + 1) * rows, :]
            left = jnp.concatenate([both[:heads], zero], axis=0)
            right = jnp.concatenate([zero, both[heads:]], axis=0)
            query = jnp.concatenate([left, right], axis=1).astype(bf16)
            keys = jnp.concatenate([kbuf[2 * p], kbuf[2 * p + 1]], axis=1)
            scores.append(dot(query, keys, ((1,), (1,))))
        taken = {}
        highs = []
        lows = []
        for i in range(len(members)):
            for c in range(blocks):
                z = scores[i][:, c * LANES : (c + 1) * LANES] * HEAD_DIM ** (-0.5) + offset
                tail = jnp.log1p(jnp.exp(-jnp.abs(z)))
                fail = jnp.where(position + c * LANES < limits[i], -(jnp.maximum(z, 0.0) + tail), 0.0)
                taken[i, c] = jnp.minimum(z, 0.0) - tail
                high, low = split_two(fail)
                highs.append(high)
                lows.append(low)
        halves = jnp.concatenate([jnp.concatenate(highs, axis=0), jnp.concatenate(lows, axis=0)], axis=1)
        sums = dot(halves, later[...])
        sticks = []
        for i in range(len(members)):
            carried = jnp.zeros((rows, LANES), f32)
            stick = [None] * blocks
            for c in reversed(range(blocks)):
                at = (i * blocks + c) * rows
                share = jnp.exp(taken[i, c] + (sums[at : at + rows, :LANES] + carried))
                stick[c] = jnp.where(position + c * LANES < limits[i], share, 0.0).astype(bf16)
                carried = carried + sums[at : at + rows, LANES:]
            sticks.append(jnp.concatenate(stick, axis=1))
        for p in members:
            value_copy(p).wait()
        for i, p in enumerate(members):
            values = jnp.concatenate([vbuf[2 * p], vbuf[2 * p + 1]], axis=1)
            attended = dot(sticks[i], values)
            arows[p * rows : (p + 1) * rows, :] = jnp.where(first, attended[:, :LANES], attended[:, LANES:])

    for members in groups:
        one_group(members)

    tiles = []
    for q in range(heads // 2):
        upper = 2 * q >= heads // 2
        even = arows[pl.ds(2 * q, seqs, stride=heads), :]
        odd = arows[pl.ds(2 * q + 1, seqs, stride=heads), :]
        if upper:
            even = pltpu.roll(even, HEAD_DIM, 1)
        else:
            odd = pltpu.roll(odd, HEAD_DIM, 1)
        tiles.append(jnp.where(lane < HEAD_DIM, even, odd))
    attended = jnp.concatenate(tiles, axis=1).astype(bf16)
    weights[3].wait()
    part_out[...] = dot(attended, wo[...]).astype(bf16)
    for copy in outs:
        copy.wait()


def attention(*args):
    caches = [pltpu.with_memory_space_constraint(x, pltpu.HBM) for x in args]
    lengths, offsets, tokens, gain, key_cache, value_cache, w_query, w_key, w_value, w_out = args
    seqs, width = tokens.shape
    heads = offsets.shape[0]
    kv = w_key.shape[1]
    vmem = pl.BlockSpec(memory_space=pltpu.VMEM)
    hbm = pl.BlockSpec(memory_space=pltpu.HBM)
    return pl.pallas_call(
        attention_kernel,
        out_shape=(
            jax.ShapeDtypeStruct((seqs, width), bf16),
            jax.ShapeDtypeStruct((seqs, kv), bf16),
            jax.ShapeDtypeStruct((seqs, kv), bf16),
        ),
        in_specs=[hbm] * len(args),
        out_specs=(vmem, hbm, hbm),
        scratch_shapes=[
            pltpu.SMEM(lengths.shape, jnp.int32),
            pltpu.SMEM(offsets.shape, f32),
            pltpu.VMEM(tokens.shape, bf16),
            pltpu.VMEM(gain.shape, f32),
            pltpu.VMEM(key_cache.shape, bf16),
            pltpu.VMEM(value_cache.shape, bf16),
            pltpu.VMEM(w_query.shape, bf16),
            pltpu.VMEM(w_key.shape, bf16),
            pltpu.VMEM(w_value.shape, bf16),
            pltpu.VMEM(w_out.shape, bf16),
            pltpu.VMEM((seqs * heads, LANES), f32),
            pltpu.VMEM((seqs * heads, LANES), f32),
            pltpu.VMEM((2 * LANES, 2 * LANES), bf16),
            pltpu.VMEM((seqs, kv), bf16),
            pltpu.VMEM((seqs, kv), bf16),
            pltpu.SemaphoreType.DMA((8,)),
            pltpu.SemaphoreType.DMA((seqs // 2,)),
            pltpu.SemaphoreType.DMA((seqs // 2,)),
            pltpu.SemaphoreType.DMA((2,)),
        ],
        compiler_params=pltpu.CompilerParams(vmem_limit_bytes=20 << 20),
        name="attention",
    )(*caches)


def dispatch_kernel(
    tokens, gain, own, peer, routes_hbm, weights_hbm, rows_out, middle_out, mix_out, route, weight, sems
):
    seqs, width = tokens.shape
    half = width // 2
    own_slots = rows_out.shape[0] // EXPERTS
    start = (lax.axis_index("plane") * lax.axis_size("spot") + lax.axis_index("spot")) * seqs
    tile = pl.multiple_of(start // LANES * LANES, LANES)
    copies = [
        pltpu.make_async_copy(routes_hbm.at[:, pl.ds(tile, LANES)], route, sems.at[0]),
        pltpu.make_async_copy(weights_hbm.at[:, pl.ds(tile, LANES)], weight, sems.at[1]),
    ]
    for copy in copies:
        copy.start()
    tp_index = lax.axis_index("tp")
    low_half = tp_index == 0
    middle = (tokens[...].astype(f32) + own[...].astype(f32) + peer[...].astype(f32)).astype(bf16)
    moe_in = rms_rows(middle, gain[...])
    middle = middle.astype(f32)
    middle_out[...] = jnp.where(low_half, middle[:, :half], middle[:, half:]).astype(bf16)
    for copy in copies:
        copy.wait()
    here = iota((seqs, LANES), 1) == iota((seqs, LANES), 0) + (start - tile)

    def column(values):
        return jnp.sum(jnp.where(here, values, 0.0), axis=1, keepdims=True)

    r0, r1 = (column(route[i : i + 1, :].astype(f32)) for i in range(2))
    w0, w1 = (column(weight[i : i + 1, :]) for i in range(2))
    earlier = jnp.where(iota((seqs, seqs), 1) < iota((seqs, seqs), 0), 1.0, 0.0).astype(bf16)

    def slot_mask(expert, slot):
        expert = expert.astype(f32)
        first = r0 == expert
        named = first | (r1 == expert)
        before = dot(earlier, jnp.where(named, 1.0, 0.0).astype(bf16))
        return first, named & (before == slot.astype(f32))

    index = iota((seqs, rows_out.shape[0]), 1)
    _, chosen = slot_mask(index // own_slots, tp_index * own_slots + index % own_slots)
    rows_out[...] = dot(jnp.where(chosen, 1.0, 0.0).astype(bf16), moe_in, ((0,), (0,))).astype(bf16)
    index = iota((seqs, mix_out.shape[1]), 1)
    source, part = index // (SIDES * own_slots), index // own_slots
    expert = source // 2 * SIDES + part % SIDES
    first, chosen = slot_mask(expert, source % 2 * own_slots + index % own_slots)
    high, low = split_two(jnp.where(chosen, jnp.where(first, w0, w1), 0.0))
    mix_out[...] = jnp.concatenate([high, low], axis=0)


def dispatch(tokens, gain, own, peer, routes, weights, capacity):
    seqs, width = tokens.shape
    vmem = pl.BlockSpec(memory_space=pltpu.VMEM)
    hbm = pl.BlockSpec(memory_space=pltpu.HBM)
    outs = ((EXPERTS * capacity // 2, width), (seqs, width // 2), (2 * seqs, EXPERTS * capacity))
    return pl.pallas_call(
        dispatch_kernel,
        out_shape=tuple(jax.ShapeDtypeStruct(shape, bf16) for shape in outs),
        in_specs=[vmem] * 4 + [hbm] * 2,
        out_specs=(vmem,) * 3,
        scratch_shapes=[
            pltpu.VMEM((2, LANES), jnp.int32),
            pltpu.VMEM((2, LANES), f32),
            pltpu.SemaphoreType.DMA((2,)),
        ],
        compiler_params=pltpu.CompilerParams(vmem_limit_bytes=8 << 20),
        name="dispatch",
    )(tokens, gain, own, peer, routes, weights)


def expert_kernel(rows, gate_own, up_own, down_own, gate_hbm, up_hbm, down_hbm, out, gate_peer, up_peer, down_peer, sems):
    peers = ((gate_hbm, gate_peer), (up_hbm, up_peer), (down_hbm, down_peer))
    copies = [pltpu.make_async_copy(src, dst, sems.at[i]) for i, (src, dst) in enumerate(peers)]
    for copy in copies:
        copy.start()
    x = rows[...]

    def hidden_of(gate, upward):
        return (gate / (1.0 + jnp.exp(-gate)) * upward).astype(bf16)

    def project(w):
        return dot(x, w, ((1,), (1,)))

    total = dot(hidden_of(project(gate_own[...]), project(up_own[...])), down_own[...])
    copies[0].wait()
    gate = project(gate_peer[...])
    copies[1].wait()
    hidden = hidden_of(gate, project(up_peer[...]))
    copies[2].wait()
    out[...] = (total + dot(hidden, down_peer[...])).astype(bf16)


def expert(rows, own, peers):
    vmem = pl.BlockSpec(memory_space=pltpu.VMEM)
    hbm = pl.BlockSpec(memory_space=pltpu.HBM)
    peers = [pltpu.with_memory_space_constraint(w, pltpu.HBM) for w in peers]
    return pl.pallas_call(
        expert_kernel,
        out_shape=jax.ShapeDtypeStruct(rows.shape, bf16),
        in_specs=[vmem] * 4 + [hbm] * 3,
        out_specs=vmem,
        scratch_shapes=[pltpu.VMEM(w.shape, bf16) for w in peers] + [pltpu.SemaphoreType.DMA((3,))],
        compiler_params=pltpu.CompilerParams(vmem_limit_bytes=16 << 20),
        name="expert",
    )(rows, *own, *peers)


def mix_kernel(mix, returned, middle, out):
    seqs = middle.shape[0]
    both = dot(mix[...], returned[...])
    out[...] = (middle[...].astype(f32) + (both[:seqs] + both[seqs:])).astype(bf16)


def mix_rows(mix, returned, middle):
    vmem = pl.BlockSpec(memory_space=pltpu.VMEM)
    return pl.pallas_call(
        mix_kernel,
        out_shape=jax.ShapeDtypeStruct(middle.shape, bf16),
        in_specs=[vmem] * 3,
        out_specs=vmem,
        compiler_params=pltpu.CompilerParams(vmem_limit_bytes=8 << 20),
        name="mix",
    )(mix, returned, middle)


def shards(
    tokens,
    lengths,
    routes,
    route_weights,
    key_cache,
    value_cache,
    w_query,
    w_key,
    w_value,
    w_out,
    score_offset,
    attn_gain,
    ffn_gain,
    w_gate,
    w_up,
    w_down,
):
    _, width = tokens.shape
    planes, plane = lax.axis_size("plane"), lax.axis_size("spot")
    capacity = 4
    half = width // 2
    swap = [(0, 1), (1, 0)]

    def named_swap(x):
        return lax.ppermute(x, "tp", swap)

    def exchange(x, axes):
        return lax.all_to_all(x, axes, 0, 0, tiled=True)

    gate_w, up_w = w_gate.T, w_up.T
    part, new_keys, new_values = attention(
        lengths,
        score_offset,
        tokens,
        attn_gain.reshape(1, width),
        key_cache,
        value_cache,
        w_query,
        w_key,
        w_value,
        w_out,
    )
    other_part = named_swap(part)
    rows, middle, mix = dispatch(
        tokens,
        ffn_gain.reshape(1, width),
        part,
        other_part,
        routes.T,
        route_weights.T,
        capacity,
    )
    own_weights = (gate_w, up_w, w_down)
    *waiting, part = lax.optimization_barrier(own_weights + (part,))
    peer_weights = [named_swap(w) for w in waiting]
    slots = capacity // 2
    landed = exchange(rows.reshape(planes, SIDES * slots, width), "plane")
    landed = landed.reshape(planes, SIDES, slots, width).transpose(1, 0, 2, 3)
    landed = landed.reshape(SIDES, 1, planes * slots, width)
    outgoing = jnp.broadcast_to(landed, (SIDES, plane // SIDES, planes * slots, width))
    arrived = exchange(outgoing.reshape(plane, planes * slots, width), "spot")
    shares = expert(arrived.reshape(plane * planes * slots, width), own_weights, peer_weights)
    landed = exchange(shares.reshape(plane, planes * slots, width), "spot")
    landed = landed.reshape(SIDES, plane // SIDES, planes * slots, width).astype(f32).sum(axis=1).astype(bf16)
    landed = landed.reshape(SIDES, planes, slots, 2, half).transpose(1, 3, 0, 2, 4)
    returned = exchange(landed.reshape(2 * planes, SIDES * slots, half), ("plane", "tp"))
    layer_out = mix_rows(mix, returned.reshape(EXPERTS * capacity, half), middle)
    return (layer_out, new_keys, new_values)


def solution(mesh):
    devices = mesh.devices
    fine = Mesh(devices.reshape(PLANES, -1, devices.shape[-1]), ("plane", "spot", "tp"))
    ep = ("plane", "spot")
    in_specs = (
        P(ep, None),
        P(ep),
        P(),
        P(),
        P(ep, None, "tp"),
        P(ep, None, "tp"),
        P(None, "tp"),
        P(None, "tp"),
        P(None, "tp"),
        P("tp", None),
        P("tp"),
        P(),
        P(),
        P(None, ep + ("tp",)),
        P(None, ep + ("tp",)),
        P(ep + ("tp",), None),
    )
    out_specs = (P(ep, "tp"), P(ep, "tp"), P(ep, "tp"))
    return jax.shard_map(shards, mesh=fine, in_specs=in_specs, out_specs=out_specs, check_vma=False)
```
